128 devices in a mesh: grp: 4 (over y, x), ep: 32 (over z, core).
Axes of the slice: x: 2, y: 2, z: 16, core: 2. Of those that a mesh axis runs over, the one named last changes fastest.
The devices are a block of a 8x8x16 slice.
Arguments:
- stream: bfloat16 [32768, 2048], P(('grp', 'ep')), parts along dimension 0, may hold values from -6 to 6
- norm_gain: float32 [2048], replicated, may hold values from 0.1 to 1.9
- routing: int32 [32768, 4], P(('grp', 'ep')), parts along dimension 0, may hold values from 0 to 63, all different within a row; in each aligned block of 256 rows (0 to 255, 256 to 511, ...) at most 32 rows name the same one
- gates: float32 [32768, 4], P(('grp', 'ep')), parts along dimension 0, may hold values from 0.1 to 1
- w_gate: bfloat16 [64, 2048, 512], P('ep'), may hold values from -0.125 to 0.125
- w_up: bfloat16 [64, 2048, 512], P('ep'), may hold values from -0.125 to 0.125
- w_down: bfloat16 [64, 512, 2048], P('ep'), may hold values from -0.25 to 0.25
- shared_gate: bfloat16 [2048, 512], replicated, may hold values from -0.125 to 0.125
- shared_up: bfloat16 [2048, 512], replicated, may hold values from -0.125 to 0.125
- shared_down: bfloat16 [512, 2048], replicated, may hold values from -0.25 to 0.25
Outputs:
- mixed: bfloat16 [32768, 2048], P(('grp', 'ep')), parts along dimension 0
The draws below stay inside these ranges and needn't reach their ends.
There are 4 independent parts, one for each index of `grp`. The reference program is written for one: setup_inputs(seed, part) draws one part's arguments, and reference() takes and returns one part's arrays. A program takes and returns all parts, laid end to end along the dimension named above; an argument that names none is the same for every part. Nothing has to cross between parts.
Inputs may be any that keep to these rules, and one draw needn't show every extreme that they name: `routing`: each token names 4 different experts. Among the 256 tokens of one index of ep no expert is named more than 32 times, and on some index an expert is named exactly 32 times.
All inputs are finite; a program needn't handle non-finite values.
Results may differ from the reference program's by a relative error of at most 0.007.
Values may be sent and summed in bfloat16 or wider, within the bound.
No kernel may reach another device: no remote copies, remote signals or barrier semaphores. Data moves between devices by JAX's collectives and lax.ppermute only.
A program may use at most 128 MiB of HBM per device.

```python
import math
import jax
import jax.numpy as jnp
import numpy as np
from jax import lax

D = 2048
DE = 512
DS = 512
TOP_K = 4
TOK_DEV = 256
TOKENS = 8192
EXPERTS = 64
CAP = 32
N_EP = 32


def block_scale(stream_key, shape, split, low, high):
    level, own = 1.0, jax.random.fold_in(stream_key, 6)
    for axis_at, blocks in split:
        draws = jnp.exp(jax.random.uniform(jax.random.fold_in(own, axis_at), (blocks,), jnp.float32, low / len(split), high / len(split)))
        level = level * jnp.repeat(draws, shape[axis_at] // blocks).reshape([-1 if axis == axis_at else 1 for axis in range(len(shape))])
    return level


def deal_out(rng, own, number, rows, count, top, most, skew):
    sequence = jax.random.permutation(rng, count)
    packed, ordinary = load_shares(count, rows * top, most, skew, True), load_shares(count, rows * top, most, skew, False)
    places = jnp.arange(count)

    def named(sizes, offset_by):
        used = int((sizes > 0).sum())
        fixed = max(1, used // 4)
        moved = fixed + (places - fixed + offset_by * (used - fixed)) % max(1, count - fixed)
        return jnp.zeros((count,), jnp.int32).at[sequence[jnp.where(places < fixed, places, moved)]].set(jnp.asarray(sizes, jnp.int32))

    sizes = jnp.where(number % 4 == 0, named(packed, number // 4), named(ordinary, number - number // 4 - 1))
    mixed = jax.random.permutation(jax.random.fold_in(own, 3), count)
    donor, sink = mixed[0:count // 2 * 2:2], mixed[1:count // 2 * 2:2]
    slack = jnp.minimum(sizes[donor] - 1, most - sizes[sink]) // 2
    slack = jnp.where((donor == sequence[0]) | (sink == sequence[0]) | (sizes[sink] == 0), 0, jnp.maximum(slack, 0))
    moved = jax.random.randint(jax.random.fold_in(own, 4), (count // 2,), 0, 1 << 20) % (slack + 1)
    sizes = sizes.at[donor].add(-moved).at[sink].add(moved)
    members = jnp.searchsorted(jnp.cumsum(sizes), jnp.arange(rows * top), side="right").astype(jnp.int32)
    table = members.reshape(top, rows).T
    table = table[jax.random.permutation(jax.random.fold_in(own, 1), rows)]
    offset_by = jax.random.randint(jax.random.fold_in(own, 2), (rows, 1), 0, top)
    return jnp.take_along_axis(table, (jnp.arange(top)[None, :] + offset_by) % top, axis=1)


def load_shares(number_of, total, limit, slope, full):
    weights = [(1 << 20) // math.isqrt(standing ** slope) + 1 for standing in range(1, number_of + 1)]
    largest = limit if full else min(limit, max(-(-total // number_of), total * weights[0] // sum(weights)))
    least = 1 if total - largest >= number_of - 1 else 0
    counts, surplus = [largest] + [least] * (number_of - 1), total - largest - least * (number_of - 1)
    while surplus > 0:
        movable = [i for i in range(1, number_of) if counts[i] < largest] or [i for i in range(1, number_of) if counts[i] < limit]
        pool, left = sum([weights[i] for i in movable]), surplus
        for i in movable:
            extra = min(limit - counts[i], max(1, left * weights[i] // pool), surplus)
            counts[i] = counts[i] + extra
            surplus = surplus - extra
    return np.array(counts)


def gaussian(own_key, shape, spread, limit, pieces=(), kind=jnp.bfloat16):
    level = block_scale(own_key, shape, pieces, -0.22, 0.18) if pieces else 1.0
    entries = jax.random.normal(own_key, shape, jnp.float32) * spread * level
    return jnp.minimum(jnp.maximum(entries, -limit), limit).astype(kind)


def setup_inputs(seed: int = 0, part: int = 0) -> dict:
    streams_of = jax.random.split(jax.random.key(seed), 11)
    own_keys = jax.random.split(jax.random.fold_in(streams_of[10], part), 11)
    stream = gaussian(own_keys[0], (TOKENS, D), 1.0, 6.0, ((0, 32),))
    norm_gain = jnp.clip(1.0 + 0.18 * jax.random.normal(streams_of[1], (D,), jnp.float32), 0.1, 1.9)
    routing_keys = jax.random.split(jax.random.fold_in(own_keys[2], 1), TOKENS // TOK_DEV)
    routing_turns = jax.random.permutation(jax.random.fold_in(own_keys[2], 3), TOKENS // TOK_DEV)
    routing = jax.vmap(lambda own, number: deal_out(jax.random.fold_in(own_keys[2], 2), own, number, TOK_DEV, EXPERTS, TOP_K, CAP, 2))(routing_keys, routing_turns).reshape((TOKENS, TOP_K))
    gates = jnp.clip(0.1 + 0.9 * jax.random.uniform(own_keys[3], (TOKENS, TOP_K), jnp.float32) ** block_scale(own_keys[3], (TOKENS, TOP_K), ((0, 32),), -0.2, 0.2), 0.1, 1.0)
    w_gate = gaussian(streams_of[4], (EXPERTS, D, DE), D ** -0.5, 0.125, ((0, 32),))
    w_up = gaussian(streams_of[5], (EXPERTS, D, DE), D ** -0.5, 0.125, ((0, 32),))
    w_down = gaussian(streams_of[6], (EXPERTS, DE, D), DE ** -0.5, 0.25, ((0, 32),))
    shared_gate = gaussian(streams_of[7], (D, DS), D ** -0.5, 0.125)
    shared_up = gaussian(streams_of[8], (D, DS), D ** -0.5, 0.125)
    shared_down = gaussian(streams_of[9], (DS, D), DS ** -0.5, 0.25)
    return {"stream": stream, "norm_gain": norm_gain, "routing": routing, "gates": gates, "w_gate": w_gate, "w_up": w_up, "w_down": w_down, "shared_gate": shared_gate, "shared_up": shared_up, "shared_down": shared_down}


def layer_norm(stream, norm_gain):
    widened = stream.astype(jnp.float32)
    row_mean = lax.optimization_barrier(jnp.mean(widened, axis=-1, keepdims=True))
    variance = lax.optimization_barrier(jnp.mean(jnp.square(widened - row_mean), axis=-1, keepdims=True))
    return ((widened - row_mean) * lax.rsqrt(variance + 1e-05) * norm_gain).astype(jnp.bfloat16)

def reference(stream, norm_gain, routing, gates, w_gate, w_up, w_down, shared_gate, shared_up, shared_down):
    normed = layer_norm(stream, norm_gain)
    flat_ids = routing.reshape(-1)
    weights = gates.reshape(-1)
    total_rows = TOKENS * TOP_K
    capacity = N_EP * CAP

    def visit_expert(running, expert):
        chosen = jnp.nonzero(flat_ids == expert, size=capacity, fill_value=total_rows)[0].astype(jnp.int32)
        usable = chosen < total_rows
        clipped = jnp.minimum(chosen, total_rows - 1)
        token_ids = clipped // TOP_K
        gathered = normed[token_ids]
        gate_act = jnp.dot(gathered, w_gate[expert], preferred_element_type=jnp.float32)
        up_act = jnp.dot(gathered, w_up[expert], preferred_element_type=jnp.float32)
        hidden = (jax.nn.silu(gate_act) * up_act).astype(jnp.bfloat16)
        produced = jnp.dot(hidden, w_down[expert], preferred_element_type=jnp.float32).astype(jnp.bfloat16)
        weight_col = jnp.where(usable, weights[clipped], jnp.float32(0.0))
        running = running.at[token_ids].add(produced.astype(jnp.float32) * weight_col[:, None])
        return (running, None)
    start = jnp.zeros((TOKENS, D), jnp.float32)
    routed, _ = lax.scan(visit_expert, start, jnp.arange(EXPERTS, dtype=jnp.int32))
    shared_hidden = (jax.nn.silu(jnp.dot(normed, shared_gate, preferred_element_type=jnp.float32)) * jnp.dot(normed, shared_up, preferred_element_type=jnp.float32)).astype(jnp.bfloat16)
    shared_out = jnp.dot(shared_hidden, shared_down, preferred_element_type=jnp.float32)
    return (routed + shared_out).astype(jnp.bfloat16)
```

```python
import jax
import jax.numpy as jnp
from jax import lax
from jax.sharding import Mesh
from jax.sharding import PartitionSpec as P

EP = ("ep_0", "ep_1")
GRP_EP = ("grp", "ep_0", "ep_1")
CHUNKS = 2


def layer_norm(stream, norm_gain):
    widened = stream.astype(jnp.float32)
    row_mean = jnp.mean(widened, axis=-1, keepdims=True)
    variance = jnp.mean(jnp.square(widened - row_mean), axis=-1, keepdims=True)
    return ((widened - row_mean) * lax.rsqrt(variance + 1e-05) * norm_gain).astype(jnp.bfloat16)


def shared_branch(normed, shared_gate, shared_up, shared_down):
    shared_hidden = (
        jax.nn.silu(jnp.dot(normed, shared_gate, preferred_element_type=jnp.float32))
        * jnp.dot(normed, shared_up, preferred_element_type=jnp.float32)
    ).astype(jnp.bfloat16)
    return jnp.dot(shared_hidden, shared_down, preferred_element_type=jnp.float32)


def served(sources, placing, slot_gates, w_gate, w_up, w_down):
    peers, rows, width = sources.shape
    local, cap = placing.shape[2], placing.shape[3]
    incoming = jnp.einsum(
        "ptxc,ptd->xpcd", placing, sources, preferred_element_type=jnp.float32
    ).astype(jnp.bfloat16).reshape(local, peers * cap, width)
    gate_act = jnp.einsum("xnd,xdh->xnh", incoming, w_gate, preferred_element_type=jnp.float32)
    up_act = jnp.einsum("xnd,xdh->xnh", incoming, w_up, preferred_element_type=jnp.float32)
    weight = slot_gates.reshape(local, peers * cap, 1)
    hidden = (jax.nn.silu(gate_act) * up_act * weight).astype(jnp.bfloat16)
    produced = jnp.einsum(
        "xnh,xhd->xnd", hidden, w_down, preferred_element_type=jnp.float32
    ).astype(jnp.bfloat16).reshape(local, peers, cap, width)
    return jnp.einsum(
        "ptxc,xpcd->ptd", placing, produced, preferred_element_type=jnp.float32
    ).astype(jnp.bfloat16)


def on_device(
    stream, norm_gain, routing, gates, w_gate, w_up, w_down, shared_gate, shared_up, shared_down
):
    tok_rows, top_count = routing.shape
    width = stream.shape[1]
    local_count = w_gate.shape[0]
    peer_count = lax.axis_size(EP)
    experts = local_count * peer_count
    capacity = 2 * tok_rows * top_count // experts
    part = tok_rows // CHUNKS
    normed = layer_norm(stream, norm_gain)
    gathered = [
        lax.all_gather(normed[i * part : (i + 1) * part], EP, axis=0, tiled=True)
        for i in range(CHUNKS)
    ]
    tags = jnp.concatenate([routing.T.astype(jnp.float32), gates.T], axis=0)
    all_tags = lax.all_gather(tags, EP, axis=0, tiled=False)
    ids, values = all_tags[:, :top_count], all_tags[:, top_count:]
    first_expert = (lax.axis_index(EP) * local_count).astype(jnp.float32)
    mine = first_expert + jnp.arange(local_count, dtype=jnp.int32).astype(jnp.float32)
    matches = (ids[:, :, :, None] == mine).astype(jnp.float32)
    hits = jnp.sum(matches, axis=1)
    weights = jnp.sum(matches * values[:, :, :, None], axis=1)
    row_ids = jnp.arange(part, dtype=jnp.int32)
    lower = (row_ids[:, None] > row_ids[None, :]).astype(jnp.bfloat16)
    slot_ids = jnp.arange(capacity, dtype=jnp.int32).astype(jnp.float32)
    returned = []
    for i in range(CHUNKS):
        chunk_hits = hits[:, i * part : (i + 1) * part]
        chunk_weights = weights[:, i * part : (i + 1) * part]
        prior = jnp.einsum(
            "ab,pbx->pax", lower, chunk_hits.astype(jnp.bfloat16), preferred_element_type=jnp.float32
        )
        placed = chunk_hits[:, :, :, None] * (prior[:, :, :, None] == slot_ids).astype(jnp.float32)
        slot_gates = jnp.sum(placed * chunk_weights[:, :, :, None], axis=1)
        sums = served(
            gathered[i].reshape(peer_count, part, width),
            placed.astype(jnp.bfloat16),
            slot_gates.transpose(1, 0, 2),
            w_gate,
            w_up,
            w_down,
        )
        returned.append(
            lax.psum_scatter(
                sums.reshape(peer_count * part, width), EP, scatter_dimension=0, tiled=True
            )
        )
    shared = shared_branch(normed, shared_gate, shared_up, shared_down)
    routed = jnp.concatenate(returned, axis=0).astype(jnp.float32)
    return (routed + shared).astype(jnp.bfloat16)


def solution(mesh):
    torus = Mesh(mesh.devices.reshape(mesh.shape["grp"], mesh.shape["ep"] // 2, 2), ("grp", "ep_0", "ep_1"))
    return jax.shard_map(
        on_device,
        mesh=torus,
        in_specs=(
            P(GRP_EP, None),
            P(),
            P(GRP_EP, None),
            P(GRP_EP, None),
            P(EP, None, None),
            P(EP, None, None),
            P(EP, None, None),
            P(),
            P(),
            P(),
        ),
        out_specs=P(GRP_EP, None),
        check_vma=False,
    )
```

```python
import functools

import jax
import jax.numpy as jnp
from jax import lax
from jax.experimental import pallas as pl
from jax.experimental.pallas import tpu as pltpu
from jax.sharding import Mesh
from jax.sharding import PartitionSpec as P

GRP_EP = ("grp", "ep_0", "ep_1")
TAG_ROWS = 8
BF16, F32 = jnp.bfloat16, jnp.float32
VMEM_BYTES = 60 * 1024 * 1024


def vmem_spec(shape):
    return pl.BlockSpec(shape, lambda *_: (0,) * len(shape))


def norm_body(stream, gain, tags, first, second):
    half = second.shape[0]
    rows = 16

    def block(source, target, i):
        x = stream[pl.ds(source + i * rows, rows), :].astype(F32)
        mean = jnp.mean(x, axis=-1, keepdims=True)
        centred = x - mean
        variance = jnp.mean(centred * centred, axis=-1, keepdims=True)
        y = centred * lax.rsqrt(variance + 1e-05) * gain[...]
        target[pl.ds(i * rows, rows), :] = y.astype(BF16)

    @pl.loop(0, half // rows)
    def _(i):
        block(0, first, i)
        block(half, second, i)

    first[half : half + TAG_ROWS, :] = tags[...]


def normed_chunks(stream, gain, tags):
    tokens, width = stream.shape
    half = tokens // 2
    return pl.pallas_call(
        norm_body,
        out_shape=(
            jax.ShapeDtypeStruct((half + TAG_ROWS, width), BF16),
            jax.ShapeDtypeStruct((half, width), BF16),
        ),
        compiler_params=pltpu.CompilerParams(vmem_limit_bytes=VMEM_BYTES),
        name="norm_chunks",
    )(stream, gain.reshape(1, width), tags)


def tag_row(first, half, tokens, index):
    width = first.shape[1]
    start = index * tokens
    row, lane = start // width, start % width
    return first[half + row : half + row + 1, lane : lane + tokens].astype(F32)


def expert_body(*refs, sources, top, cap, final):
    bases = refs[0]
    at = 1
    chunks = [(refs[at + 2 * s], refs[at + 2 * s + 1]) for s in range(sources)]
    at += 2 * sources
    w_gate, w_up, w_down = refs[at : at + 3]
    at += 3
    if final:
        earlier = refs[at]
        at += 1
        outs = [(refs[at + 2 * s], refs[at + 2 * s + 1]) for s in range(sources)]
        at += 2 * sources
    else:
        produced = refs[at]
        at += 1
    picked, slot_gates, placing, sums = refs[at : at + 4]
    at += 4
    if final:
        produced = refs[at]
    expert, piece = pl.program_id(0), pl.program_id(1)
    local, pieces = pl.num_programs(0), pl.num_programs(1)
    half = chunks[0][1].shape[0]
    tokens = 2 * half
    local_count = picked.shape[0]
    groups = 2 if final else 1

    @pl.when((expert == 0) & (piece == 0))
    def _():
        hit_rows, gate_rows = [], []
        for s in range(sources):
            first = chunks[s][0]
            ids = [tag_row(first, half, tokens, k) for k in range(top)]
            values = [
                tag_row(first, half, tokens, top + k) + tag_row(first, half, tokens, 2 * top + k)
                for k in range(top)
            ]
            for g in range(groups):
                for x in range(local_count):
                    wanted = (bases[g] + x).astype(F32)
                    hit, value = 0.0, 0.0
                    for k in range(top):
                        match = jnp.where(ids[k] == wanted, 1.0, 0.0)
                        hit = hit + match
                        value = value + match * values[k]
                    hit_rows.append(hit)
                    gate_rows.append(value)
        count = len(hit_rows)
        padded = -(-count // 16) * 16
        stacked = jnp.concatenate(
            hit_rows + [jnp.zeros((padded - count, tokens), F32)] * (padded > count), axis=0
        )
        before = (
            lax.broadcasted_iota(jnp.int32, (tokens, tokens), 0)
            < lax.broadcasted_iota(jnp.int32, (tokens, tokens), 1)
        )
        ranks = jnp.dot(
            stacked.astype(BF16), jnp.where(before, 1.0, 0.0).astype(BF16), preferred_element_type=F32
        )
        slot = lax.broadcasted_iota(jnp.int32, (cap, tokens), 0).astype(F32)
        for s in range(sources):
            for g in range(groups):
                for x in range(local_count):
                    n = (s * groups + g) * local_count + x
                    chosen = jnp.where(
                        (ranks[n : n + 1, :] == slot) & (hit_rows[n] > 0.5), 1.0, 0.0
                    )
                    placing[s, (g * local_count + x) * cap : (g * local_count + x + 1) * cap, :] = (
                        chosen.astype(BF16)
                    )
                    if g == groups - 1:
                        column = jnp.sum(chosen * gate_rows[n], axis=1, keepdims=True)
                        slot_gates[x, s * cap : (s + 1) * cap, :] = jnp.broadcast_to(
                            column, (cap, slot_gates.shape[2])
                        )
        low = (groups - 1) * local_count * cap
        for s in range(sources):
            first, second = chunks[s]
            mask = placing[s, low : low + local_count * cap, :]
            rows = jnp.dot(mask[:, :half], first[:half, :], preferred_element_type=F32) + jnp.dot(
                mask[:, half:], second[...], preferred_element_type=F32
            )
            rows = rows.astype(BF16)
            for x in range(local_count):
                picked[x, s * cap : (s + 1) * cap, :] = rows[x * cap : (x + 1) * cap, :]

    rows = picked[expert]
    gate_act = jnp.dot(rows, w_gate[0], preferred_element_type=F32)
    up_act = jnp.dot(rows, w_up[0], preferred_element_type=F32)
    weight = slot_gates[expert][:, :1]
    hidden = (gate_act / (1.0 + jnp.exp(-gate_act)) * up_act * weight).astype(BF16)
    part = jnp.dot(hidden, w_down[0], preferred_element_type=F32)

    @pl.when(piece == 0)
    def _():
        sums[...] = part

    @pl.when(piece > 0)
    def _():
        sums[...] += part

    @pl.when(piece == pieces - 1)
    def _():
        for s in range(sources):
            produced[s, pl.ds(expert * cap, cap), :] = sums[s * cap : (s + 1) * cap, :].astype(BF16)

    if final:

        @pl.when((expert == local - 1) & (piece == pieces - 1))
        def _():
            span = local_count * cap
            contract = (((0,), (0,)), ((), ()))
            for s in range(sources):
                for side in range(2):
                    lanes = slice(side * half, (side + 1) * half)
                    total = lax.dot_general(
                        placing[s, :span, lanes], earlier[s], contract, preferred_element_type=F32
                    ) + lax.dot_general(
                        placing[s, span:, lanes], produced[s], contract, preferred_element_type=F32
                    )
                    outs[s][side][...] = total.astype(BF16)


def expert_call(bases, chunks, weights, earlier, top, cap, pieces=2):
    sources = len(chunks)
    w_gate, w_up, w_down = weights
    local_count, width, hidden = w_gate.shape
    block = hidden // pieces
    half = chunks[0][1].shape[0]
    final = earlier is not None
    groups = 2 if final else 1
    flat = [part for pair in chunks for part in pair]
    out_slots = jax.ShapeDtypeStruct((sources, local_count * cap, width), BF16)
    in_specs = (
        [pl.BlockSpec(memory_space=pltpu.SMEM)]
        + [vmem_spec(part.shape) for part in flat]
        + [
            pl.BlockSpec((1, width, block), lambda x, j: (x, 0, j)),
            pl.BlockSpec((1, width, block), lambda x, j: (x, 0, j)),
            pl.BlockSpec((1, block, width), lambda x, j: (x, j, 0)),
        ]
    )
    operands = [bases, *flat, w_gate, w_up, w_down]
    scratch = [
        pltpu.VMEM((local_count, sources * cap, width), BF16),
        pltpu.VMEM((local_count, sources * cap, 128), F32),
        pltpu.VMEM((sources, groups * local_count * cap, 2 * half), BF16),
        pltpu.VMEM((sources * cap, width), F32),
    ]
    if final:
        in_specs.append(vmem_spec(out_slots.shape))
        operands.append(earlier)
        out_shape = [jax.ShapeDtypeStruct((half, width), BF16)] * (2 * sources)
        scratch.append(pltpu.VMEM(out_slots.shape, BF16))
    else:
        out_shape = [out_slots]
    result = pl.pallas_call(
        functools.partial(expert_body, sources=sources, top=top, cap=cap, final=final),
        grid=(local_count, pieces),
        in_specs=in_specs,
        out_specs=[vmem_spec(o.shape) for o in out_shape],
        out_shape=out_shape,
        scratch_shapes=scratch,
        compiler_params=pltpu.CompilerParams(vmem_limit_bytes=VMEM_BYTES),
        cost_estimate=pl.CostEstimate(
            flops=2 * 3 * local_count * 256 * width * hidden,
            bytes_accessed=2 * 3 * local_count * width * hidden + sources * 4 * half * width,
            transcendentals=local_count * sources * cap * hidden,
        ),
        name="expert_final" if final else "expert_first",
    )(*operands)
    if final:
        return [(result[2 * s], result[2 * s + 1]) for s in range(sources)]
    return result[0]


def shared_branch(normed, shared_gate, shared_up, shared_down):
    shared_hidden = (
        jax.nn.silu(jnp.dot(normed, shared_gate, preferred_element_type=F32))
        * jnp.dot(normed, shared_up, preferred_element_type=F32)
    ).astype(BF16)
    return jnp.dot(shared_hidden, shared_down, preferred_element_type=F32)


def tag_table(routing, gates, width):
    high = lax.reduce_precision(gates, 8, 7)
    low = gates - high
    table = jnp.concatenate([routing.T.astype(F32), high.T, low.T], axis=0).astype(BF16).reshape(-1)
    return jnp.pad(table, (0, TAG_ROWS * width - table.shape[0])).reshape(TAG_ROWS, width)


def on_device(
    stream, norm_gain, routing, gates, w_gate, w_up, w_down, shared_gate, shared_up, shared_down
):
    tokens, width = stream.shape
    top = routing.shape[1]
    half = tokens // 2
    local_count = w_gate.shape[0]
    ring, cores = lax.axis_size("ep_0"), lax.axis_size("ep_1")
    cap = 2 * tokens * top // (local_count * ring * cores)
    place, core = lax.axis_index("ep_0"), lax.axis_index("ep_1")
    base = (place * cores + core) * local_count
    other = (place * cores + (cores - 1 - core)) * local_count
    first_bases = jnp.stack([base, other]).astype(jnp.int32)
    rightward = [(i, (i + 1) % ring) for i in range(ring)]
    leftward = [(i, (i - 1) % ring) for i in range(ring)]
    swap = [(0, 1), (1, 0)]
    far = ring // 2

    own = (w_gate, w_up, w_down)
    theirs = tuple(lax.ppermute(w, "ep_1", swap) for w in own)
    chunk_a, chunk_b = normed_chunks(stream, norm_gain, tag_table(routing, gates, width))

    own_pair = (chunk_a, chunk_b)
    held = {("own", 0): own_pair, ("r", 0): own_pair, ("l", 0): own_pair}
    shares = {}

    def sent(parts, side, hop, gate=None):
        if gate is not None:
            parts, _ = lax.optimization_barrier((parts, gate))
        right, left = parts
        if hop == far:
            return lax.ppermute(right if side == 0 else left, "ep_0", rightward if side == 0 else leftward)
        return lax.ppermute(right, "ep_0", rightward), lax.ppermute(left, "ep_0", leftward)

    batches = {2: [("own", 0), ("r", 1), ("l", 1), ("r", 2), ("l", 2)]}
    for hop in range(4, far, 2):
        batches[hop] = [(d, h) for h in (hop - 1, hop) for d in ("r", "l")]
    last = [("r", far - 1), ("l", far - 1), ("far", far)]
    for hop in range(1, far + 1):
        batch = batches.get(hop - 2)
        before = (held["r", hop - 1], held["l", hop - 1])
        gate = None
        if batch is not None:
            chunks = [held[key] for key in batch]
            slots = expert_call(first_bases, chunks, own, None, top, cap)
            gate = slots
        a = sent((before[0][0], before[1][0]), 0, hop, gate)
        if batch is not None:
            pairs = expert_call(first_bases, chunks, theirs, slots, top, cap)
            shares.update(zip(batch, pairs))
            gate = pairs[0][0]
        b = sent((before[0][1], before[1][1]), 1, hop, gate)
        if hop == far:
            held["far", far] = (a, b)
        else:
            held["r", hop], held["l", hop] = (a[0], b[0]), (a[1], b[1])
    chunks = [held[key] for key in last]
    slots = expert_call(first_bases, chunks, own, None, top, cap)
    shares.update(zip(last, expert_call(first_bases, chunks, theirs, slots, top, cap)))

    def joined(moving, share):
        return (moving.astype(F32) + share.astype(F32)).astype(BF16)

    back_ra, back_lb = shares["far", far]
    back_rb, back_la = None, None
    for hop in range(far - 1, 0, -1):
        back_ra = joined(lax.ppermute(back_ra, "ep_0", leftward), shares["r", hop][0])
        if back_la is None:
            back_la, back_rb = shares["l", hop][0], shares["r", hop][1]
        else:
            back_la = joined(lax.ppermute(back_la, "ep_0", rightward), shares["l", hop][0])
            back_rb = joined(lax.ppermute(back_rb, "ep_0", leftward), shares["r", hop][1])
        back_lb = joined(lax.ppermute(back_lb, "ep_0", rightward), shares["l", hop][1])
    ends = [
        (lax.ppermute(back_ra, "ep_0", leftward), lax.ppermute(back_la, "ep_0", rightward)),
        (lax.ppermute(back_rb, "ep_0", leftward), lax.ppermute(back_lb, "ep_0", rightward)),
    ]
    normed = jnp.concatenate([chunk_a[:half], chunk_b], axis=0)
    shared = shared_branch(normed, shared_gate, shared_up, shared_down)
    mixed = [
        (
            from_r.astype(F32)
            + from_l.astype(F32)
            + shares["own", 0][i].astype(F32)
            + shared[i * half : (i + 1) * half]
        ).astype(BF16)
        for i, (from_r, from_l) in enumerate(ends)
    ]
    return jnp.concatenate(mixed, axis=0)


def solution(mesh):
    ring = mesh.shape["ep"] // 2
    torus = Mesh(mesh.devices.reshape(mesh.shape["grp"], ring, 2), ("grp", "ep_0", "ep_1"))
    ep = ("ep_0", "ep_1")
    return jax.shard_map(
        on_device,
        mesh=torus,
        in_specs=(
            P(GRP_EP, None),
            P(),
            P(GRP_EP, None),
            P(GRP_EP, None),
            P(ep, None, None),
            P(ep, None, None),
            P(ep, None, None),
            P(),
            P(),
            P(),
        ),
        out_specs=P(GRP_EP, None),
        check_vma=False,
    )
```

```python
import functools

import jax
import jax.numpy as jnp
from jax import lax
from jax.experimental import pallas as pl
from jax.experimental.pallas import tpu as pltpu
from jax.sharding import Mesh
from jax.sharding import PartitionSpec as P

GRP_EP = ("grp", "ep_0", "ep_1")
TAG_ROWS = 8
BF16, F32 = jnp.bfloat16, jnp.float32
VMEM_BYTES = 60 * 1024 * 1024


def vmem_spec(shape):
    return pl.BlockSpec(shape, lambda *_: (0,) * len(shape))


def norm_body(stream, gain, tags, first, second):
    half = second.shape[0]
    rows = 16

    def block(source, target, i):
        x = stream[pl.ds(source + i * rows, rows), :].astype(F32)
        mean = jnp.mean(x, axis=-1, keepdims=True)
        centred = x - mean
        variance = jnp.mean(centred * centred, axis=-1, keepdims=True)
        y = centred * lax.rsqrt(variance + 1e-05) * gain[...]
        target[pl.ds(i * rows, rows), :] = y.astype(BF16)

    @pl.loop(0, half // rows)
    def _(i):
        block(0, first, i)
        block(half, second, i)

    first[half : half + TAG_ROWS, :] = tags[...]


def normed_chunks(stream, gain, tags):
    tokens, width = stream.shape
    half = tokens // 2
    return pl.pallas_call(
        norm_body,
        out_shape=(
            jax.ShapeDtypeStruct((half + TAG_ROWS, width), BF16),
            jax.ShapeDtypeStruct((half, width), BF16),
        ),
        compiler_params=pltpu.CompilerParams(vmem_limit_bytes=VMEM_BYTES),
        name="norm_chunks",
    )(stream, gain.reshape(1, width), tags)


def tag_row(first, half, tokens, index):
    width = first.shape[1]
    start = index * tokens
    row, lane = start // width, start % width
    return first[half + row : half + row + 1, lane : lane + tokens].astype(F32)


def expert_body(*refs, sources, top, cap, sets, local, whole):
    ids = refs[0]
    at = 1
    chunks = [(refs[at + 2 * s], refs[at + 2 * s + 1]) for s in range(sources)]
    at += 2 * sources
    weights = [refs[at + 3 * g : at + 3 * g + 3] for g in range(sets)]
    at += 3 * sets
    if whole:
        outs = [(refs[at + 2 * s], refs[at + 2 * s + 1]) for s in range(sources)]
        at += 2 * sources
        picked, slot_gates, sums, placing, produced = refs[at:]
    else:
        produced, placing, picked, slot_gates, sums = refs[at:]
    expert, piece = pl.program_id(0), pl.program_id(1)
    pieces = pl.num_programs(1)
    half = chunks[0][1].shape[0]
    tokens = 2 * half
    count = sets * local

    @pl.when((expert == 0) & (piece == 0))
    def _():
        hit_rows, gate_rows = [], []
        for s in range(sources):
            first = chunks[s][0]
            named = [tag_row(first, half, tokens, k) for k in range(top)]
            values = [
                tag_row(first, half, tokens, top + k) + tag_row(first, half, tokens, 2 * top + k)
                for k in range(top)
            ]
            for x in range(count):
                wanted = ids[x].astype(F32)
                hit, value = 0.0, 0.0
                for k in range(top):
                    match = jnp.where(named[k] == wanted, 1.0, 0.0)
                    hit = hit + match
                    value = value + match * values[k]
                hit_rows.append(hit)
                gate_rows.append(value)
        padded = -(-len(hit_rows) // 16) * 16
        fill = [jnp.zeros((padded - len(hit_rows), tokens), F32)] * (padded > len(hit_rows))
        stacked = jnp.concatenate(hit_rows + fill, axis=0)
        before = (
            lax.broadcasted_iota(jnp.int32, (tokens, tokens), 0)
            < lax.broadcasted_iota(jnp.int32, (tokens, tokens), 1)
        )
        ranks = jnp.dot(
            stacked.astype(BF16), jnp.where(before, 1.0, 0.0).astype(BF16), preferred_element_type=F32
        )
        slot = lax.broadcasted_iota(jnp.int32, (cap, tokens), 0).astype(F32)
        for s in range(sources):
            for x in range(count):
                n = s * count + x
                chosen = jnp.where((ranks[n : n + 1, :] == slot) & (hit_rows[n] > 0.5), 1.0, 0.0)
                placing[s, x * cap : (x + 1) * cap, :] = chosen.astype(BF16)
                column = jnp.sum(chosen * gate_rows[n], axis=1, keepdims=True)
                slot_gates[x, s * cap : (s + 1) * cap, :] = jnp.broadcast_to(
                    column, (cap, slot_gates.shape[2])
                )
        for s in range(sources):
            first, second = chunks[s]
            mask = placing[s]
            rows = jnp.dot(mask[:, :half], first[:half, :], preferred_element_type=F32) + jnp.dot(
                mask[:, half:], second[...], preferred_element_type=F32
            )
            rows = rows.astype(BF16)
            for x in range(count):
                picked[x, s * cap : (s + 1) * cap, :] = rows[x * cap : (x + 1) * cap, :]

    def step(w_gate, w_up, w_down):
        rows = picked[expert]
        gate_act = jnp.dot(rows, w_gate[0], preferred_element_type=F32)
        up_act = jnp.dot(rows, w_up[0], preferred_element_type=F32)
        weight = slot_gates[expert][:, :1]
        hidden = (gate_act / (1.0 + jnp.exp(-gate_act)) * up_act * weight).astype(BF16)
        part = jnp.dot(hidden, w_down[0], preferred_element_type=F32)

        @pl.when(piece == 0)
        def _():
            sums[...] = part

        @pl.when(piece > 0)
        def _():
            sums[...] += part

    for g in range(sets):
        if sets == 1:
            step(*weights[g])
        else:
            pl.when((expert >= g * local) & (expert < (g + 1) * local))(
                functools.partial(step, *weights[g])
            )

    @pl.when(piece == pieces - 1)
    def _():
        if whole:
            for s in range(sources):
                produced[s, pl.ds(expert * cap, cap), :] = sums[s * cap : (s + 1) * cap, :].astype(BF16)
        else:
            produced[...] = sums[...].astype(BF16)

    if whole:

        @pl.when((expert == count - 1) & (piece == pieces - 1))
        def _():
            for s in range(sources):
                for side in range(2):
                    total = lax.dot_general(
                        placing[s, :, side * half : (side + 1) * half],
                        produced[s],
                        (((0,), (0,)), ((), ())),
                        preferred_element_type=F32,
                    )
                    outs[s][side][...] = total.astype(BF16)


def expert_call(ids, chunks, weights, cap, top, only=None, pieces=2):
    sources, sets = len(chunks), len(weights)
    local_count, width, hidden = weights[0][0].shape
    block = hidden // pieces
    half = chunks[0][1].shape[0]
    whole = only is None
    local = local_count if whole else 1
    count = sets * local
    flat = [part for pair in chunks for part in pair]

    def at(g, dim):
        def index(x, j):
            if whole:
                early, late = x < g * local, x >= (g + 1) * local
                j = jnp.where(early, 0, jnp.where(late, pieces - 1, j))
                x = jnp.clip(x - g * local, 0, local - 1)
            else:
                x = only
            return (x, 0, j) if dim == 2 else (x, j, 0)

        return index

    weight_specs = []
    for g in range(sets):
        weight_specs += [
            pl.BlockSpec((1, width, block), at(g, 2)),
            pl.BlockSpec((1, width, block), at(g, 2)),
            pl.BlockSpec((1, block, width), at(g, 1)),
        ]
    scratch = [
        pltpu.VMEM((count, sources * cap, width), BF16),
        pltpu.VMEM((count, sources * cap, 128), F32),
        pltpu.VMEM((sources * cap, width), F32),
    ]
    if whole:
        out_shape = [jax.ShapeDtypeStruct((half, width), BF16)] * (2 * sources)
        scratch += [
            pltpu.VMEM((sources, count * cap, 2 * half), BF16),
            pltpu.VMEM((sources, count * cap, width), BF16),
        ]
    else:
        out_shape = [
            jax.ShapeDtypeStruct((sources * cap, width), BF16),
            jax.ShapeDtypeStruct((sources, cap, 2 * half), BF16),
        ]
    return pl.pallas_call(
        functools.partial(
            expert_body, sources=sources, top=top, cap=cap, sets=sets, local=local, whole=whole
        ),
        grid=(count, pieces),
        in_specs=[pl.BlockSpec(memory_space=pltpu.SMEM)]
        + [vmem_spec(part.shape) for part in flat]
        + weight_specs,
        out_specs=[vmem_spec(o.shape) for o in out_shape],
        out_shape=out_shape,
        scratch_shapes=scratch,
        compiler_params=pltpu.CompilerParams(vmem_limit_bytes=VMEM_BYTES),
        cost_estimate=pl.CostEstimate(
            flops=2 * 3 * count * 256 * width * hidden,
            bytes_accessed=2 * 3 * count * width * hidden + sources * 4 * half * width,
            transcendentals=count * sources * cap * hidden,
        ),
        name="experts_whole" if whole else "expert_rows",
    )(ids, *flat, *[w for group in weights for w in group])


def fold_body(*refs, count):
    moving, rows, masks, out = refs[0], refs[1 : 1 + count], refs[1 + count : 1 + 2 * count], refs[-1]
    mask = jnp.concatenate([m[0] for m in masks], axis=0)
    total = lax.dot_general(
        mask,
        jnp.concatenate([r[...] for r in rows], axis=0),
        (((0,), (0,)), ((), ())),
        preferred_element_type=F32,
    )
    out[...] = (moving[...].astype(F32) + total).astype(BF16)


def folded(moving, served, source, side, cap):
    half, width = moving.shape
    count = len(served)
    return pl.pallas_call(
        functools.partial(fold_body, count=count),
        grid=(1,),
        in_specs=[vmem_spec((half, width))]
        + [pl.BlockSpec((cap, width), lambda i: (source, 0))] * count
        + [pl.BlockSpec((1, cap, half), lambda i: (source, 0, side))] * count,
        out_specs=vmem_spec((half, width)),
        out_shape=jax.ShapeDtypeStruct((half, width), BF16),
        compiler_params=pltpu.CompilerParams(vmem_limit_bytes=VMEM_BYTES),
        cost_estimate=pl.CostEstimate(
            flops=2 * count * cap * half * width,
            bytes_accessed=4 * half * width + 2 * count * cap * width,
            transcendentals=0,
        ),
        name="fold",
    )(moving, *[rows for rows, _ in served], *[mask for _, mask in served])


def close_body(*refs, count):
    shared = refs[0]
    moving = refs[1:5]
    rows, masks, out = refs[5 : 5 + count], refs[5 + count : 5 + 2 * count], refs[-1]
    half = moving[0].shape[0]
    block = jnp.concatenate([r[...] for r in rows], axis=0)
    for side in range(2):
        lanes = slice(side * half, (side + 1) * half)
        mask = jnp.concatenate([m[0, :, lanes] for m in masks], axis=0)
        total = lax.dot_general(mask, block, (((0,), (0,)), ((), ())), preferred_element_type=F32)
        total = total + shared[lanes, :]
        total = total + moving[2 * side][...].astype(F32) + moving[2 * side + 1][...].astype(F32)
        out[lanes, :] = total.astype(BF16)


def closed(shared, moving, served, source, cap, blocks=4):
    tokens, width = shared.shape
    half, part = tokens // 2, width // blocks
    count = len(served)
    return pl.pallas_call(
        functools.partial(close_body, count=count),
        grid=(blocks,),
        in_specs=[pl.BlockSpec((tokens, part), lambda i: (0, i))]
        + [pl.BlockSpec((half, part), lambda i: (0, i))] * 4
        + [pl.BlockSpec((cap, part), lambda i: (source, i))] * count
        + [pl.BlockSpec((1, cap, tokens), lambda i: (source, 0, 0))] * count,
        out_specs=pl.BlockSpec((tokens, part), lambda i: (0, i)),
        out_shape=jax.ShapeDtypeStruct((tokens, width), BF16),
        compiler_params=pltpu.CompilerParams(vmem_limit_bytes=VMEM_BYTES),
        name="close",
    )(shared, *moving, *[rows for rows, _ in served], *[mask for _, mask in served])


def shared_branch(normed, shared_gate, shared_up, shared_down):
    shared_hidden = (
        jax.nn.silu(jnp.dot(normed, shared_gate, preferred_element_type=F32))
        * jnp.dot(normed, shared_up, preferred_element_type=F32)
    ).astype(BF16)
    return jnp.dot(shared_hidden, shared_down, preferred_element_type=F32)


def tag_table(routing, gates, width):
    high = lax.reduce_precision(gates, 8, 7)
    low = gates - high
    table = jnp.concatenate([routing.T.astype(F32), high.T, low.T], axis=0).astype(BF16).reshape(-1)
    return jnp.pad(table, (0, TAG_ROWS * width - table.shape[0])).reshape(TAG_ROWS, width)


def on_device(
    stream, norm_gain, routing, gates, w_gate, w_up, w_down, shared_gate, shared_up, shared_down
):
    tokens, width = stream.shape
    top = routing.shape[1]
    half = tokens // 2
    local_count = w_gate.shape[0]
    ring, cores = lax.axis_size("ep_0"), lax.axis_size("ep_1")
    cap = 2 * tokens * top // (local_count * ring * cores)
    place, core = lax.axis_index("ep_0"), lax.axis_index("ep_1")
    base = (place * cores + core) * local_count
    other = (place * cores + (cores - 1 - core)) * local_count
    ids = [base + x for x in range(local_count)] + [other + x for x in range(local_count)]
    ids = jnp.stack(ids).astype(jnp.int32)
    rightward = [(i, (i + 1) % ring) for i in range(ring)]
    leftward = [(i, (i - 1) % ring) for i in range(ring)]
    swap = [(0, 1), (1, 0)]
    far = ring // 2

    own = (w_gate, w_up, w_down)
    theirs = tuple(lax.ppermute(w, "ep_1", swap) for w in own)
    chunk_a, chunk_b = normed_chunks(stream, norm_gain, tag_table(routing, gates, width))

    own_pair = (chunk_a, chunk_b)
    held = {("own", 0): own_pair, ("r", 0): own_pair, ("l", 0): own_pair}
    normed = jnp.concatenate([chunk_a[:half], chunk_b], axis=0)
    shared = shared_branch(normed, shared_gate, shared_up, shared_down)

    def sent(parts, side, hop, gate=None):
        if gate is not None:
            parts, _ = lax.optimization_barrier((parts, gate))
        right, left = parts
        if hop == far:
            return lax.ppermute(right if side == 0 else left, "ep_0", rightward if side == 0 else leftward)
        return lax.ppermute(right, "ep_0", rightward), lax.ppermute(left, "ep_0", leftward)

    batches = {2: [("own", 0), ("r", 1), ("l", 1), ("r", 2), ("l", 2)]}
    for hop in range(4, far, 2):
        batches[hop] = [(d, h) for h in (hop - 1, hop) for d in ("r", "l")]
    last = [("r", far - 1), ("l", far - 1), ("far", far)]
    count = 2 * local_count
    served, where, waiting = {}, {}, []

    def serve():
        end, i = waiting.pop(0)
        chunks = [held[key] for key in batches[end]]
        group = own if i < local_count else theirs
        served[end].append(expert_call(ids[i : i + 1], chunks, (group,), cap, top, only=i % local_count))
        return served[end][-1]

    for hop in range(1, far + 1):
        if hop - 2 in batches:
            served[hop - 2] = []
            waiting += [(hop - 2, i) for i in range(count)]
            for n, key in enumerate(batches[hop - 2]):
                where[key] = (hop - 2, n)
        sides = []
        for side in range(2):
            gate = shared if hop == 2 and side == 0 else None
            if waiting:
                gate = serve()
            parts = (held["r", hop - 1][side], held["l", hop - 1][side])
            sides.append(sent(parts, side, hop, gate))
        if hop == far:
            held["far", far] = tuple(sides)
        else:
            held["r", hop], held["l", hop] = zip(*sides)
    rest = [serve() for _ in list(waiting)]
    if rest:
        held["far", far], _ = lax.optimization_barrier((held["far", far], rest))
    chunks = [held[key] for key in last]
    flat = expert_call(ids, chunks, (own, theirs), cap, top)
    shares = {key: (flat[2 * n], flat[2 * n + 1]) for n, key in enumerate(last)}

    def joined(moving, direction, hop, side):
        if moving is None:
            return shares[direction, hop][side]
        if (direction, hop) in shares:
            return (moving.astype(F32) + shares[direction, hop][side].astype(F32)).astype(BF16)
        end, source = where[direction, hop]
        return folded(moving, served[end], source, side, cap)

    streams = {("r", 0): shares["far", far][0], ("l", 1): shares["far", far][1], ("l", 0): None, ("r", 1): None}
    home = {"r": leftward, "l": rightward}
    order = [("r", 0), ("l", 0), ("r", 1), ("l", 1)]
    for hop in range(far - 1, -1, -1):
        for direction, side in order:
            moving = streams[direction, side]
            if moving is not None:
                moving = lax.ppermute(moving, "ep_0", home[direction])
            if hop > 0:
                moving = joined(moving, direction, hop, side)
            streams[direction, side] = moving
    end, source = where["own", 0]
    return closed(shared, [streams[key] for key in order], served[end], source, cap)


def solution(mesh):
    ring = mesh.shape["ep"] // 2
    torus = Mesh(mesh.devices.reshape(mesh.shape["grp"], ring, 2), ("grp", "ep_0", "ep_1"))
    ep = ("ep_0", "ep_1")
    return jax.shard_map(
        on_device,
        mesh=torus,
        in_specs=(
            P(GRP_EP, None),
            P(),
            P(GRP_EP, None),
            P(GRP_EP, None),
            P(ep, None, None),
            P(ep, None, None),
            P(ep, None, None),
            P(),
            P(),
            P(),
        ),
        out_specs=P(GRP_EP, None),
        check_vma=False,
    )
```

```python
import functools

import jax
import jax.numpy as jnp
from jax import lax
from jax.experimental import pallas as pl
from jax.experimental.pallas import tpu as pltpu
from jax.sharding import Mesh
from jax.sharding import PartitionSpec as P


GRP_EP = ("grp", "ep_0", "ep_1")
TAG_ROWS = 8
BF16, F32 = jnp.bfloat16, jnp.float32
VMEM_BYTES = 60 * 1024 * 1024


def vmem_spec(shape):
    return pl.BlockSpec(shape, lambda *_: (0,) * len(shape))


def norm_body(stream, gain, *rest):
    out = rest[-1]
    half = stream.shape[0]
    rows = 16

    @pl.loop(0, half // rows)
    def _(i):
        x = stream[pl.ds(i * rows, rows), :].astype(F32)
        mean = jnp.mean(x, axis=-1, keepdims=True)
        centred = x - mean
        variance = jnp.mean(centred * centred, axis=-1, keepdims=True)
        y = centred * lax.rsqrt(variance + 1e-05) * gain[...]
        out[pl.ds(i * rows, rows), :] = y.astype(BF16)

    if len(rest) > 1:
        out[half : half + TAG_ROWS, :] = rest[0][...]


def normed_chunk(stream, gain, side, tags=None):
    tokens, width = stream.shape
    half = tokens // 2
    extra = [] if tags is None else [tags]
    rows = half + TAG_ROWS * len(extra)
    return pl.pallas_call(
        norm_body,
        grid=(1,),
        in_specs=[pl.BlockSpec((half, width), lambda i: (side, 0)), vmem_spec((1, width))]
        + [vmem_spec(t.shape) for t in extra],
        out_specs=vmem_spec((rows, width)),
        out_shape=jax.ShapeDtypeStruct((rows, width), BF16),
        compiler_params=pltpu.CompilerParams(vmem_limit_bytes=VMEM_BYTES),
        name="norm_chunk",
    )(stream, gain.reshape(1, width), *extra)


def tag_row(chunk, half, tokens, index):
    width = chunk.shape[1]
    start = index * tokens
    row, lane = start // width, start % width
    return chunk[half + row : half + row + 1, lane : lane + tokens].astype(F32)


def expert_body(*refs, sources, top, cap, sets, local, whole):
    ids = refs[0]
    at = 1
    chunks = [(refs[at + 2 * s], refs[at + 2 * s + 1]) for s in range(sources)]
    at += 2 * sources
    weights = [refs[at + 3 * g : at + 3 * g + 3] for g in range(sets)]
    at += 3 * sets
    if whole:
        outs = [(refs[at + 2 * s], refs[at + 2 * s + 1]) for s in range(sources)]
        at += 2 * sources
        picked, slot_gates, sums, placing, produced = refs[at:]
    else:
        produced, placing, picked, slot_gates, sums = refs[at:]
    expert, piece = pl.program_id(0), pl.program_id(1)
    pieces = pl.num_programs(1)
    half = chunks[0][0].shape[0]
    tokens = 2 * half
    count = sets * local

    @pl.when((expert == 0) & (piece == 0))
    def _():
        hit_rows, gate_rows = [], []
        for s in range(sources):
            tagged = chunks[s][1]
            named = [tag_row(tagged, half, tokens, k) for k in range(top)]
            values = [
                tag_row(tagged, half, tokens, top + k) + tag_row(tagged, half, tokens, 2 * top + k)
                for k in range(top)
            ]
            for x in range(count):
                wanted = ids[x].astype(F32)
                hit, value = 0.0, 0.0
                for k in range(top):
                    match = jnp.where(named[k] == wanted, 1.0, 0.0)
                    hit = hit + match
                    value = value + match * values[k]
                hit_rows.append(hit)
                gate_rows.append(value)
        padded = -(-len(hit_rows) // 16) * 16
        fill = [jnp.zeros((padded - len(hit_rows), tokens), F32)] * (padded > len(hit_rows))
        stacked = jnp.concatenate(hit_rows + fill, axis=0)
        before = (
            lax.broadcasted_iota(jnp.int32, (tokens, tokens), 0)
            < lax.broadcasted_iota(jnp.int32, (tokens, tokens), 1)
        )
        ranks = jnp.dot(
            stacked.astype(BF16), jnp.where(before, 1.0, 0.0).astype(BF16), preferred_element_type=F32
        )
        slot = lax.broadcasted_iota(jnp.int32, (cap, tokens), 0).astype(F32)
        for s in range(sources):
            for x in range(count):
                n = s * count + x
                chosen = jnp.where((ranks[n : n + 1, :] == slot) & (hit_rows[n] > 0.5), 1.0, 0.0)
                placing[s, x * cap : (x + 1) * cap, :] = chosen.astype(BF16)
                column = jnp.sum(chosen * gate_rows[n], axis=1, keepdims=True)
                slot_gates[x, s * cap : (s + 1) * cap, :] = jnp.broadcast_to(
                    column, (cap, slot_gates.shape[2])
                )
        for s in range(sources):
            first, second = chunks[s]
            mask = placing[s]
            rows = jnp.dot(mask[:, :half], first[...], preferred_element_type=F32) + jnp.dot(
                mask[:, half:], second[:half, :], preferred_element_type=F32
            )
            rows = rows.astype(BF16)
            for x in range(count):
                picked[x, s * cap : (s + 1) * cap, :] = rows[x * cap : (x + 1) * cap, :]

    def step(w_gate, w_up, w_down):
        rows = picked[expert]
        gate_act = jnp.dot(rows, w_gate[0], preferred_element_type=F32)
        up_act = jnp.dot(rows, w_up[0], preferred_element_type=F32)
        weight = slot_gates[expert][:, :1]
        hidden = (gate_act / (1.0 + jnp.exp(-gate_act)) * up_act * weight).astype(BF16)
        part = jnp.dot(hidden, w_down[0], preferred_element_type=F32)

        @pl.when(piece == 0)
        def _():
            sums[...] = part

        @pl.when(piece > 0)
        def _():
            sums[...] += part

    for g in range(sets):
        if sets == 1:
            step(*weights[g])
        else:
            pl.when((expert >= g * local) & (expert < (g + 1) * local))(
                functools.partial(step, *weights[g])
            )

    @pl.when(piece == pieces - 1)
    def _():
        if whole:
            for s in range(sources):
                produced[s, pl.ds(expert * cap, cap), :] = sums[s * cap : (s + 1) * cap, :].astype(BF16)
        else:
            produced[...] = sums[...].astype(BF16)

    if whole:

        @pl.when((expert == count - 1) & (piece == pieces - 1))
        def _():
            for s in range(sources):
                for side in range(2):
                    total = lax.dot_general(
                        placing[s, :, side * half : (side + 1) * half],
                        produced[s],
                        (((0,), (0,)), ((), ())),
                        preferred_element_type=F32,
                    )
                    outs[s][side][...] = total.astype(BF16)


def expert_call(ids, chunks, weights, cap, top, only=None, pieces=2):
    sources, sets = len(chunks), len(weights)
    local_count, width, hidden = weights[0][0].shape
    block = hidden // pieces
    half = chunks[0][0].shape[0]
    whole = only is None
    local = local_count if whole else 1
    count = sets * local
    flat = [part for pair in chunks for part in pair]

    def at(g, dim):
        def index(x, j):
            if whole:
                early, late = x < g * local, x >= (g + 1) * local
                j = jnp.where(early, 0, jnp.where(late, pieces - 1, j))
                x = jnp.clip(x - g * local, 0, local - 1)
            else:
                x = only
            return (x, 0, j) if dim == 2 else (x, j, 0)

        return index

    weight_specs = []
    for g in range(sets):
        weight_specs += [
            pl.BlockSpec((1, width, block), at(g, 2)),
            pl.BlockSpec((1, width, block), at(g, 2)),
            pl.BlockSpec((1, block, width), at(g, 1)),
        ]
    scratch = [
        pltpu.VMEM((count, sources * cap, width), BF16),
        pltpu.VMEM((count, sources * cap, 128), F32),
        pltpu.VMEM((sources * cap, width), F32),
    ]
    if whole:
        out_shape = [jax.ShapeDtypeStruct((half, width), BF16)] * (2 * sources)
        scratch += [
            pltpu.VMEM((sources, count * cap, 2 * half), BF16),
            pltpu.VMEM((sources, count * cap, width), BF16),
        ]
    else:
        out_shape = [
            jax.ShapeDtypeStruct((sources * cap, width), BF16),
            jax.ShapeDtypeStruct((sources, cap, 2 * half), BF16),
        ]
    return pl.pallas_call(
        functools.partial(
            expert_body, sources=sources, top=top, cap=cap, sets=sets, local=local, whole=whole
        ),
        grid=(count, pieces),
        in_specs=[pl.BlockSpec(memory_space=pltpu.SMEM)]
        + [vmem_spec(part.shape) for part in flat]
        + weight_specs,
        out_specs=[vmem_spec(o.shape) for o in out_shape],
        out_shape=out_shape,
        scratch_shapes=scratch,
        compiler_params=pltpu.CompilerParams(vmem_limit_bytes=VMEM_BYTES),
        cost_estimate=pl.CostEstimate(
            flops=2 * 3 * count * 256 * width * hidden,
            bytes_accessed=2 * 3 * count * width * hidden + sources * 4 * half * width,
            transcendentals=count * sources * cap * hidden,
        ),
        name="experts_whole" if whole else "expert_rows",
    )(ids, *flat, *[w for group in weights for w in group])


def fold_body(*refs, count):
    moving, rows, masks, out = refs[0], refs[1 : 1 + count], refs[1 + count : 1 + 2 * count], refs[-1]
    mask = jnp.concatenate([m[0] for m in masks], axis=0)
    total = lax.dot_general(
        mask,
        jnp.concatenate([r[...] for r in rows], axis=0),
        (((0,), (0,)), ((), ())),
        preferred_element_type=F32,
    )
    out[...] = (moving[...].astype(F32) + total).astype(BF16)


def folded(moving, served, source, side, cap):
    half, width = moving.shape
    count = len(served)
    return pl.pallas_call(
        functools.partial(fold_body, count=count),
        grid=(1,),
        in_specs=[vmem_spec((half, width))]
        + [pl.BlockSpec((cap, width), lambda i: (source, 0))] * count
        + [pl.BlockSpec((1, cap, half), lambda i: (source, 0, side))] * count,
        out_specs=vmem_spec((half, width)),
        out_shape=jax.ShapeDtypeStruct((half, width), BF16),
        compiler_params=pltpu.CompilerParams(vmem_limit_bytes=VMEM_BYTES),
        cost_estimate=pl.CostEstimate(
            flops=2 * count * cap * half * width,
            bytes_accessed=4 * half * width + 2 * count * cap * width,
            transcendentals=0,
        ),
        name="fold",
    )(moving, *[rows for rows, _ in served], *[mask for _, mask in served])


def rest_body(*refs, count):
    shared, moving = refs[0], refs[1:3]
    rows, masks, out = refs[3 : 3 + count], refs[3 + count : 3 + 2 * count], refs[-1]
    half = moving[0].shape[0]
    block = jnp.concatenate([r[...] for r in rows], axis=0)
    for side in range(2):
        lanes = slice(side * half, (side + 1) * half)
        mask = jnp.concatenate([m[0, :, lanes] for m in masks], axis=0)
        total = lax.dot_general(mask, block, (((0,), (0,)), ((), ())), preferred_element_type=F32)
        out[lanes, :] = total + shared[lanes, :] + moving[side][...].astype(F32)


def rest_of(shared, moving, served, source, cap, blocks=4):
    tokens, width = shared.shape
    half, part = tokens // 2, width // blocks
    count = len(served)
    return pl.pallas_call(
        functools.partial(rest_body, count=count),
        grid=(blocks,),
        in_specs=[pl.BlockSpec((tokens, part), lambda i: (0, i))]
        + [pl.BlockSpec((half, part), lambda i: (0, i))] * 2
        + [pl.BlockSpec((cap, part), lambda i: (source, i))] * count
        + [pl.BlockSpec((1, cap, tokens), lambda i: (source, 0, 0))] * count,
        out_specs=pl.BlockSpec((tokens, part), lambda i: (0, i)),
        out_shape=jax.ShapeDtypeStruct((tokens, width), F32),
        compiler_params=pltpu.CompilerParams(vmem_limit_bytes=VMEM_BYTES),
        name="rest",
    )(shared, *moving, *[rows for rows, _ in served], *[mask for _, mask in served])


def close_body(rest, upper, lower, out):
    half = upper.shape[0]
    out[:half, :] = (rest[:half, :] + upper[...].astype(F32)).astype(BF16)
    out[half:, :] = (rest[half:, :] + lower[...].astype(F32)).astype(BF16)


def closed(rest, upper, lower, blocks=4):
    tokens, width = rest.shape
    half, part = tokens // 2, width // blocks
    return pl.pallas_call(
        close_body,
        grid=(blocks,),
        in_specs=[pl.BlockSpec((tokens, part), lambda i: (0, i))]
        + [pl.BlockSpec((half, part), lambda i: (0, i))] * 2,
        out_specs=pl.BlockSpec((tokens, part), lambda i: (0, i)),
        out_shape=jax.ShapeDtypeStruct((tokens, width), BF16),
        compiler_params=pltpu.CompilerParams(vmem_limit_bytes=VMEM_BYTES),
        name="close",
    )(rest, upper, lower)


def shared_hidden_of(normed, shared_gate, shared_up):
    return (
        jax.nn.silu(jnp.dot(normed, shared_gate, preferred_element_type=F32))
        * jnp.dot(normed, shared_up, preferred_element_type=F32)
    ).astype(BF16)


def tag_table(routing, gates, width):
    high = lax.reduce_precision(gates, 8, 7)
    low = gates - high
    table = jnp.concatenate([routing.T.astype(F32), high.T, low.T], axis=0).astype(BF16).reshape(-1)
    return jnp.pad(table, (0, TAG_ROWS * width - table.shape[0])).reshape(TAG_ROWS, width)


def layer(
    stream, norm_gain, routing, gates, w_gate, w_up, w_down, shared_gate, shared_up, shared_down
):
    tokens, width = stream.shape
    top = routing.shape[1]
    half = tokens // 2
    local_count = w_gate.shape[0]
    ring, cores = lax.axis_size("ep_0"), lax.axis_size("ep_1")
    cap = 2 * tokens * top // (local_count * ring * cores)
    place, core = lax.axis_index("ep_0"), lax.axis_index("ep_1")
    base = (place * cores + core) * local_count
    other = (place * cores + (cores - 1 - core)) * local_count
    ids = [base + x for x in range(local_count)] + [other + x for x in range(local_count)]
    ids = jnp.stack(ids).astype(jnp.int32)
    rightward = [(i, (i + 1) % ring) for i in range(ring)]
    leftward = [(i, (i - 1) % ring) for i in range(ring)]
    swap = [(0, 1), (1, 0)]
    far = ring // 2

    own = (w_gate, w_up, w_down)
    theirs = tuple(lax.ppermute(w, "ep_1", swap) for w in own)
    chunk_a = normed_chunk(stream, norm_gain, 0)
    (later, named, valued), _ = lax.optimization_barrier(((stream, routing, gates), chunk_a))
    chunk_b = normed_chunk(later, norm_gain, 1, tag_table(named, valued, width))

    own_pair = (chunk_a, chunk_b)
    held = {("own", 0): own_pair, ("r", 0): own_pair, ("l", 0): own_pair}
    normed = jnp.concatenate([chunk_a, chunk_b[:half]], axis=0)
    shared_hidden = lax.optimization_barrier(shared_hidden_of(normed, shared_gate, shared_up))
    shared = jnp.dot(shared_hidden, shared_down, preferred_element_type=F32)

    def sent(parts, side, hop, gate=None):
        if gate is not None:
            parts, _ = lax.optimization_barrier((parts, gate))
        right, left = parts
        if hop == far:
            return lax.ppermute(
                right if side == 0 else left, "ep_0", rightward if side == 0 else leftward
            )
        return lax.ppermute(right, "ep_0", rightward), lax.ppermute(left, "ep_0", leftward)

    batches = {1: [("own", 0), ("r", 1), ("l", 1)]}
    for hop in range(3, far - 2, 2):
        batches[hop] = [(d, h) for h in (hop - 1, hop) for d in ("r", "l")]
    near = [(d, h) for h in range(max(batches) + 1, far) for d in ("r", "l")]
    count = 2 * local_count
    served, where, waiting = {}, {}, []

    def serve():
        end, i = waiting.pop(0)
        chunks = [held[key] for key in batches[end]]
        group = own if i < local_count else theirs
        served[end].append(
            expert_call(ids[i : i + 1], chunks, (group,), cap, top, only=i % local_count)
        )
        return served[end][-1]

    for hop in range(1, far + 1):
        if hop - 2 in batches:
            served[hop - 2] = []
            waiting += [(hop - 2, i) for i in range(count)]
            for n, key in enumerate(batches[hop - 2]):
                where[key] = (hop - 2, n)
        sides = []
        for side in range(2):
            gate = (shared_hidden, shared)[side] if hop == 2 else None
            if waiting:
                gate = serve()
            parts = (held["r", hop - 1][side], held["l", hop - 1][side])
            sides.append(sent(parts, side, hop, gate))
        if hop == far:
            held["far", far] = tuple(sides)
        else:
            held["r", hop], held["l", hop] = zip(*sides)
    rest = [serve() for _ in list(waiting)]
    pairs = [held[key] for key in near]
    if rest:
        pairs, _ = lax.optimization_barrier((pairs, rest))
    flat = expert_call(ids, pairs, (own, theirs), cap, top)
    shares = {key: (flat[2 * n], flat[2 * n + 1]) for n, key in enumerate(near)}
    pair, _ = lax.optimization_barrier((held["far", far], flat))
    shares["far", far] = tuple(expert_call(ids, [pair], (own, theirs), cap, top))

    def joined(moving, direction, hop, side):
        if moving is None:
            return shares[direction, hop][side]
        if (direction, hop) in shares:
            return (moving.astype(F32) + shares[direction, hop][side].astype(F32)).astype(BF16)
        end, source = where[direction, hop]
        return folded(moving, served[end], source, side, cap)

    streams = {("r", 0): shares["far", far][0], ("l", 1): shares["far", far][1], ("l", 0): None, ("r", 1): None}
    home = {"r": leftward, "l": rightward}
    order = [("l", 0), ("r", 1), ("r", 0), ("l", 1)]
    for hop in range(far - 1, -1, -1):
        for direction, side in order:
            moving = streams[direction, side]
            if moving is not None:
                moving = lax.ppermute(moving, "ep_0", home[direction])
            if hop > 0:
                moving = joined(moving, direction, hop, side)
            streams[direction, side] = moving
    end, source = where["own", 0]
    rest = rest_of(shared, [streams["l", 0], streams["r", 1]], served[end], source, cap)
    return closed(rest, streams["r", 0], streams["l", 1])


def solution(mesh):
    ring = mesh.shape["ep"] // 2
    torus = Mesh(mesh.devices.reshape(mesh.shape["grp"], ring, 2), ("grp", "ep_0", "ep_1"))
    ep = ("ep_0", "ep_1")
    return jax.shard_map(
        layer,
        mesh=torus,
        in_specs=(
            P(GRP_EP, None),
            P(),
            P(GRP_EP, None),
            P(GRP_EP, None),
            P(ep, None, None),
            P(ep, None, None),
            P(ep, None, None),
            P(),
            P(),
            P(),
        ),
        out_specs=P(GRP_EP, None),
        check_vma=False,
    )
```

```python
import functools

import jax
import jax.numpy as jnp
from jax import lax
from jax.experimental import pallas as pl
from jax.experimental.pallas import tpu as pltpu
from jax.sharding import Mesh
from jax.sharding import PartitionSpec as P


GRP_EP = ("grp", "ep_0", "ep_1")
TAG_ROWS = 8
COLUMNS = 1024
BF16, F32 = jnp.bfloat16, jnp.float32
VMEM_BYTES = 60 * 1024 * 1024


def vmem_spec(shape):
    return pl.BlockSpec(shape, lambda *_: (0,) * len(shape))


def norm_body(stream, gain, *rest):
    out = rest[-1]
    half = stream.shape[0]
    rows = 16

    @pl.loop(0, half // rows, unroll=4)
    def _(i):
        x = stream[pl.ds(i * rows, rows), :].astype(F32)
        mean = jnp.mean(x, axis=-1, keepdims=True)
        centred = x - mean
        variance = jnp.mean(centred * centred, axis=-1, keepdims=True)
        y = centred * lax.rsqrt(variance + 1e-05) * gain[...]
        out[pl.ds(i * rows, rows), :] = y.astype(BF16)

    if len(rest) > 1:
        out[half : half + TAG_ROWS, :] = rest[0][...]


def normed_chunk(stream, gain, side, tags=None):
    tokens, width = stream.shape
    half = tokens // 2
    extra = [] if tags is None else [tags]
    rows = half + TAG_ROWS * len(extra)
    return pl.pallas_call(
        norm_body,
        grid=(1,),
        in_specs=[pl.BlockSpec((half, width), lambda i: (side, 0)), vmem_spec((1, width))]
        + [vmem_spec(t.shape) for t in extra],
        out_specs=vmem_spec((rows, width)),
        out_shape=jax.ShapeDtypeStruct((rows, width), BF16),
        compiler_params=pltpu.CompilerParams(vmem_limit_bytes=VMEM_BYTES),
        name="norm_chunk",
    )(stream, gain.reshape(1, width), *extra)


def tag_row(chunk, half, tokens, index):
    width = chunk.shape[1]
    start = index * tokens
    row, lane = start // width, start % width
    return chunk[half + row : half + row + 1, lane : lane + tokens].astype(F32)


def expert_body(*refs, sources, top, cap, sets, local, whole):
    ids = refs[0]
    at = 1
    chunks = [(refs[at + 2 * s], refs[at + 2 * s + 1]) for s in range(sources)]
    at += 2 * sources
    weights = [refs[at + 3 * g : at + 3 * g + 3] for g in range(sets)]
    at += 3 * sets
    if whole:
        outs = [(refs[at + 2 * s], refs[at + 2 * s + 1]) for s in range(sources)]
        at += 2 * sources
        picked, slot_gates, sums, placing, produced = refs[at:]
    else:
        produced, placing, picked, slot_gates, sums = refs[at:]
    expert, piece = pl.program_id(0), pl.program_id(1)
    pieces = pl.num_programs(1)
    half = chunks[0][0].shape[0]
    tokens = 2 * half
    count = sets * local
    width = picked.shape[2]
    columns_at_once = width if whole else min(width, COLUMNS)

    @pl.when((expert == 0) & (piece == 0))
    def _():
        hit_rows, gate_rows = [], []
        for s in range(sources):
            tagged = chunks[s][1]
            named = [tag_row(tagged, half, tokens, k) for k in range(top)]
            values = [
                tag_row(tagged, half, tokens, top + k) + tag_row(tagged, half, tokens, 2 * top + k)
                for k in range(top)
            ]
            for x in range(count):
                wanted = ids[x].astype(F32)
                hit, value = 0.0, 0.0
                for k in range(top):
                    match = jnp.where(named[k] == wanted, 1.0, 0.0)
                    hit = hit + match
                    value = value + match * values[k]
                hit_rows.append(hit)
                gate_rows.append(value)
        padded = -(-len(hit_rows) // 16) * 16
        fill = [jnp.zeros((padded - len(hit_rows), tokens), F32)] * (padded > len(hit_rows))
        stacked = jnp.concatenate(hit_rows + fill, axis=0)
        before = (
            lax.broadcasted_iota(jnp.int32, (tokens, tokens), 0)
            < lax.broadcasted_iota(jnp.int32, (tokens, tokens), 1)
        )
        ranks = jnp.dot(
            stacked.astype(BF16), jnp.where(before, 1.0, 0.0).astype(BF16), preferred_element_type=F32
        )
        slot = lax.broadcasted_iota(jnp.int32, (cap, tokens), 0).astype(F32)
        for s in range(sources):
            for x in range(count):
                n = s * count + x
                chosen = jnp.where((ranks[n : n + 1, :] == slot) & (hit_rows[n] > 0.5), 1.0, 0.0)
                placing[s, x * cap : (x + 1) * cap, :] = chosen.astype(BF16)
                column = jnp.sum(chosen * gate_rows[n], axis=1, keepdims=True)
                slot_gates[x, s * cap : (s + 1) * cap, :] = jnp.broadcast_to(
                    column, (cap, slot_gates.shape[2])
                )
        for s in range(sources):
            first, second = chunks[s]
            mask = placing[s]

            @pl.loop(0, width // columns_at_once)
            def _(n, s=s, first=first, second=second, mask=mask):
                columns = pl.ds(n * columns_at_once, columns_at_once)
                rows = jnp.dot(mask[:, :half], first[:, columns], preferred_element_type=F32) + jnp.dot(
                    mask[:, half:], second[:half, columns], preferred_element_type=F32
                )
                rows = rows.astype(BF16)
                for x in range(count):
                    picked[x, s * cap : (s + 1) * cap, columns] = rows[x * cap : (x + 1) * cap, :]

    def step(w_gate, w_up, w_down):
        rows = picked[expert]
        gate_act = jnp.dot(rows, w_gate[0], preferred_element_type=F32)
        up_act = jnp.dot(rows, w_up[0], preferred_element_type=F32)
        weight = slot_gates[expert][:, :1]
        hidden = (gate_act / (1.0 + jnp.exp(-gate_act)) * up_act * weight).astype(BF16)

        @pl.when(piece == 0)
        def _():
            sums[...] = jnp.zeros(sums.shape, F32)

        @pl.loop(0, width // columns_at_once)
        def _(n):
            columns = pl.ds(n * columns_at_once, columns_at_once)
            sums[:, columns] += jnp.dot(hidden, w_down[0, :, columns], preferred_element_type=F32)

    for g in range(sets):
        if sets == 1:
            step(*weights[g])
        else:
            pl.when((expert >= g * local) & (expert < (g + 1) * local))(
                functools.partial(step, *weights[g])
            )

    @pl.when(piece == pieces - 1)
    def _():
        if whole:
            for s in range(sources):
                produced[s, pl.ds(expert * cap, cap), :] = sums[s * cap : (s + 1) * cap, :].astype(BF16)
        else:
            produced[...] = sums[...].astype(BF16)

    if whole:

        @pl.when((expert == count - 1) & (piece == pieces - 1))
        def _():
            for s in range(sources):
                for side in range(2):

                    @pl.loop(0, width // columns_at_once)
                    def _(n, s=s, side=side):
                        columns = pl.ds(n * columns_at_once, columns_at_once)
                        total = lax.dot_general(
                            placing[s, :, side * half : (side + 1) * half],
                            produced[s, :, columns],
                            (((0,), (0,)), ((), ())),
                            preferred_element_type=F32,
                        )
                        outs[s][side][:, columns] = total.astype(BF16)


def expert_call(ids, chunks, weights, cap, top, only=None, pieces=2):
    sources, sets = len(chunks), len(weights)
    local_count, width, hidden = weights[0][0].shape
    block = hidden // pieces
    half = chunks[0][0].shape[0]
    whole = only is None
    local = local_count if whole else 1
    count = sets * local
    flat = [part for pair in chunks for part in pair]

    def at(g, dim):
        def index(x, j):
            if whole:
                early, late = x < g * local, x >= (g + 1) * local
                j = jnp.where(early, 0, jnp.where(late, pieces - 1, j))
                x = jnp.clip(x - g * local, 0, local - 1)
            else:
                x = only
            return (x, 0, j) if dim == 2 else (x, j, 0)

        return index

    weight_specs = []
    for g in range(sets):
        weight_specs += [
            pl.BlockSpec((1, width, block), at(g, 2)),
            pl.BlockSpec((1, width, block), at(g, 2)),
            pl.BlockSpec((1, block, width), at(g, 1)),
        ]
    scratch = [
        pltpu.VMEM((count, sources * cap, width), BF16),
        pltpu.VMEM((count, sources * cap, 128), F32),
        pltpu.VMEM((sources * cap, width), F32),
    ]
    if whole:
        out_shape = [jax.ShapeDtypeStruct((half, width), BF16)] * (2 * sources)
        scratch += [
            pltpu.VMEM((sources, count * cap, 2 * half), BF16),
            pltpu.VMEM((sources, count * cap, width), BF16),
        ]
    else:
        out_shape = [
            jax.ShapeDtypeStruct((sources * cap, width), BF16),
            jax.ShapeDtypeStruct((sources, cap, 2 * half), BF16),
        ]
    return pl.pallas_call(
        functools.partial(
            expert_body, sources=sources, top=top, cap=cap, sets=sets, local=local, whole=whole
        ),
        grid=(count, pieces),
        in_specs=[pl.BlockSpec(memory_space=pltpu.SMEM)]
        + [vmem_spec(part.shape) for part in flat]
        + weight_specs,
        out_specs=[vmem_spec(o.shape) for o in out_shape],
        out_shape=out_shape,
        scratch_shapes=scratch,
        compiler_params=pltpu.CompilerParams(vmem_limit_bytes=VMEM_BYTES),
        cost_estimate=pl.CostEstimate(
            flops=2 * 3 * count * 256 * width * hidden,
            bytes_accessed=2 * 3 * count * width * hidden + sources * 4 * half * width,
            transcendentals=count * sources * cap * hidden,
        ),
        name="experts_whole" if whole else "expert_rows",
    )(ids, *flat, *[w for group in weights for w in group])


def fold_body(*refs, count):
    moving, rows, masks, out = refs[0], refs[1 : 1 + count], refs[1 + count : 1 + 2 * count], refs[-1]
    mask = jnp.concatenate([m[0] for m in masks], axis=0)
    total = lax.dot_general(
        mask,
        jnp.concatenate([r[...] for r in rows], axis=0),
        (((0,), (0,)), ((), ())),
        preferred_element_type=F32,
    )
    out[...] = (moving[...].astype(F32) + total).astype(BF16)


def folded(moving, served, source, side, cap, blocks=4):
    half, width = moving.shape
    count = len(served)
    return pl.pallas_call(
        functools.partial(fold_body, count=count),
        grid=(blocks,),
        in_specs=[pl.BlockSpec((half, width // blocks), lambda i: (0, i))]
        + [pl.BlockSpec((cap, width // blocks), lambda i: (source, i))] * count
        + [pl.BlockSpec((1, cap, half), lambda i: (source, 0, side))] * count,
        out_specs=pl.BlockSpec((half, width // blocks), lambda i: (0, i)),
        out_shape=jax.ShapeDtypeStruct((half, width), BF16),
        compiler_params=pltpu.CompilerParams(vmem_limit_bytes=VMEM_BYTES),
        cost_estimate=pl.CostEstimate(
            flops=2 * count * cap * half * width,
            bytes_accessed=4 * half * width + 2 * count * cap * width,
            transcendentals=0,
        ),
        name="fold",
    )(moving, *[rows for rows, _ in served], *[mask for _, mask in served])


def rest_body(*refs, count):
    shared, moving = refs[0], refs[1:3]
    rows, masks, out = refs[3 : 3 + count], refs[3 + count : 3 + 2 * count], refs[-1]
    half = moving[0].shape[0]
    block = jnp.concatenate([r[...] for r in rows], axis=0)
    for side in range(2):
        lanes = slice(side * half, (side + 1) * half)
        mask = jnp.concatenate([m[0, :, lanes] for m in masks], axis=0)
        total = lax.dot_general(mask, block, (((0,), (0,)), ((), ())), preferred_element_type=F32)
        out[lanes, :] = total + shared[lanes, :] + moving[side][...].astype(F32)


def rest_of(shared, moving, served, source, cap, blocks=4):
    tokens, width = shared.shape
    half, part = tokens // 2, width // blocks
    count = len(served)
    return pl.pallas_call(
        functools.partial(rest_body, count=count),
        grid=(blocks,),
        in_specs=[pl.BlockSpec((tokens, part), lambda i: (0, i))]
        + [pl.BlockSpec((half, part), lambda i: (0, i))] * 2
        + [pl.BlockSpec((cap, part), lambda i: (source, i))] * count
        + [pl.BlockSpec((1, cap, tokens), lambda i: (source, 0, 0))] * count,
        out_specs=pl.BlockSpec((tokens, part), lambda i: (0, i)),
        out_shape=jax.ShapeDtypeStruct((tokens, width), F32),
        compiler_params=pltpu.CompilerParams(vmem_limit_bytes=VMEM_BYTES),
        name="rest",
    )(shared, *moving, *[rows for rows, _ in served], *[mask for _, mask in served])


def close_body(rest, upper, lower, out):
    half = upper.shape[0]
    out[:half, :] = (rest[:half, :] + upper[...].astype(F32)).astype(BF16)
    out[half:, :] = (rest[half:, :] + lower[...].astype(F32)).astype(BF16)


def closed(rest, upper, lower, blocks=4):
    tokens, width = rest.shape
    half, part = tokens // 2, width // blocks
    return pl.pallas_call(
        close_body,
        grid=(blocks,),
        in_specs=[pl.BlockSpec((tokens, part), lambda i: (0, i))]
        + [pl.BlockSpec((half, part), lambda i: (0, i))] * 2,
        out_specs=pl.BlockSpec((tokens, part), lambda i: (0, i)),
        out_shape=jax.ShapeDtypeStruct((tokens, width), BF16),
        compiler_params=pltpu.CompilerParams(vmem_limit_bytes=VMEM_BYTES),
        name="close",
    )(rest, upper, lower)


def shared_hidden_of(normed, shared_gate, shared_up):
    return (
        jax.nn.silu(jnp.dot(normed, shared_gate, preferred_element_type=F32))
        * jnp.dot(normed, shared_up, preferred_element_type=F32)
    ).astype(BF16)


def tag_table(routing, gates, width):
    high = lax.reduce_precision(gates, 8, 7)
    low = gates - high
    table = jnp.concatenate([routing.T.astype(F32), high.T, low.T], axis=0).astype(BF16).reshape(-1)
    return jnp.pad(table, (0, TAG_ROWS * width - table.shape[0])).reshape(TAG_ROWS, width)


def layer(
    stream, norm_gain, routing, gates, w_gate, w_up, w_down, shared_gate, shared_up, shared_down
):
    tokens, width = stream.shape
    top = routing.shape[1]
    half = tokens // 2
    local_count = w_gate.shape[0]
    ring, cores = lax.axis_size("ep_0"), lax.axis_size("ep_1")
    cap = 2 * tokens * top // (local_count * ring * cores)
    place, core = lax.axis_index("ep_0"), lax.axis_index("ep_1")
    base = (place * cores + core) * local_count
    other = (place * cores + (cores - 1 - core)) * local_count
    ids = [base + x for x in range(local_count)] + [other + x for x in range(local_count)]
    ids = jnp.stack(ids).astype(jnp.int32)
    rightward = [(i, (i + 1) % ring) for i in range(ring)]
    leftward = [(i, (i - 1) % ring) for i in range(ring)]
    swap = [(0, 1), (1, 0)]
    far = ring // 2

    own = (w_gate, w_up, w_down)
    theirs = tuple(lax.ppermute(w, "ep_1", swap) for w in own)
    chunk_a = normed_chunk(stream, norm_gain, 0)
    (later, named, valued), _ = lax.optimization_barrier(((stream, routing, gates), chunk_a))
    chunk_b = normed_chunk(later, norm_gain, 1, tag_table(named, valued, width))

    own_pair = (chunk_a, chunk_b)
    held = {("own", 0): own_pair, ("r", 0): own_pair, ("l", 0): own_pair}
    normed = jnp.concatenate([chunk_a, chunk_b[:half]], axis=0)
    shared_hidden = lax.optimization_barrier(shared_hidden_of(normed, shared_gate, shared_up))
    shared = jnp.dot(shared_hidden, shared_down, preferred_element_type=F32)

    def sent(parts, side, hop, gate=None):
        if gate is not None:
            parts, _ = lax.optimization_barrier((parts, gate))
        right, left = parts
        if hop == far:
            return lax.ppermute(
                right if side == 0 else left, "ep_0", rightward if side == 0 else leftward
            )
        return lax.ppermute(right, "ep_0", rightward), lax.ppermute(left, "ep_0", leftward)

    batches = {1: [("own", 0), ("r", 1), ("l", 1)]}
    for hop in range(3, far - 2, 2):
        batches[hop] = [(d, h) for h in (hop - 1, hop) for d in ("r", "l")]
    near = [(d, h) for h in range(max(batches) + 1, far) for d in ("r", "l")]
    count = 2 * local_count
    served, where, waiting = {}, {}, []

    def serve():
        end, i = waiting.pop(0)
        chunks = [held[key] for key in batches[end]]
        group = own if i < local_count else theirs
        served[end].append(
            expert_call(ids[i : i + 1], chunks, (group,), cap, top, only=i % local_count)
        )
        return served[end][-1]

    for hop in range(1, far + 1):
        if hop - 2 in batches:
            served[hop - 2] = []
            waiting += [(hop - 2, i) for i in range(count)]
            for n, key in enumerate(batches[hop - 2]):
                where[key] = (hop - 2, n)
        sides = []
        for side in range(2):
            gate = (shared_hidden, shared)[side] if hop == 2 else None
            if waiting:
                gate = serve()
            parts = (held["r", hop - 1][side], held["l", hop - 1][side])
            sides.append(sent(parts, side, hop, gate))
        if hop == far:
            held["far", far] = tuple(sides)
        else:
            held["r", hop], held["l", hop] = zip(*sides)
    rest = [serve() for _ in list(waiting)]
    pairs = [held[key] for key in near]
    if rest:
        pairs, _ = lax.optimization_barrier((pairs, rest))
    flat = expert_call(ids, pairs, (own, theirs), cap, top)
    shares = {key: (flat[2 * n], flat[2 * n + 1]) for n, key in enumerate(near)}
    pair, _ = lax.optimization_barrier((held["far", far], flat))
    shares["far", far] = tuple(expert_call(ids, [pair], (own, theirs), cap, top))

    def joined(moving, direction, hop, side):
        if moving is None:
            return shares[direction, hop][side]
        if (direction, hop) in shares:
            return (moving.astype(F32) + shares[direction, hop][side].astype(F32)).astype(BF16)
        end, source = where[direction, hop]
        return folded(moving, served[end], source, side, cap)

    streams = {("r", 0): shares["far", far][0], ("l", 1): shares["far", far][1], ("l", 0): None, ("r", 1): None}
    home = {"r": leftward, "l": rightward}
    order = [("l", 0), ("r", 1), ("r", 0), ("l", 1)]
    for hop in range(far - 1, -1, -1):
        for direction, side in order:
            moving = streams[direction, side]
            if moving is not None:
                moving = lax.ppermute(moving, "ep_0", home[direction])
            if hop > 0:
                moving = joined(moving, direction, hop, side)
            streams[direction, side] = moving
    end, source = where["own", 0]
    rest = rest_of(shared, [streams["l", 0], streams["r", 1]], served[end], source, cap)
    return closed(rest, streams["r", 0], streams["l", 1])


def solution(mesh):
    ring = mesh.shape["ep"] // 2
    torus = Mesh(mesh.devices.reshape(mesh.shape["grp"], ring, 2), ("grp", "ep_0", "ep_1"))
    ep = ("ep_0", "ep_1")
    return jax.shard_map(
        layer,
        mesh=torus,
        in_specs=(
            P(GRP_EP, None),
            P(),
            P(GRP_EP, None),
            P(GRP_EP, None),
            P(ep, None, None),
            P(ep, None, None),
            P(ep, None, None),
            P(),
            P(),
            P(),
        ),
        out_specs=P(GRP_EP, None),
        check_vma=False,
    )
```
